32 devices in a mesh: sp: 8 (over z, y), tp: 4 (over x, core).
Axes of the slice: x: 2, y: 2, z: 4, core: 2. Of those that a mesh axis runs over, the one named last changes fastest.
Arguments:
- q_proj: bfloat16 [4096, 1024], P('sp', 'tp'), may hold values from -5.25 to 5.25
- k_proj: bfloat16 [4096, 512], P('sp', 'tp'), may hold values from -5.25 to 5.25
- v_proj: bfloat16 [4096, 512], P('sp', 'tp'), may hold values from -6 to 6
- doc_ids: int32 [4096], P('sp'), may hold values from 0 to 3, never falling along the last dimension, each value on 1 to 2048 neighbouring positions
- sinks: float32 [16], P('tp'), may hold values from 0.5 to 5.5
- resid: bfloat16 [4096, 2048], P(('sp', 'tp')), may hold values from -12 to 12
- w_out: bfloat16 [1024, 2048], P('tp'), may hold values from -4 to 4
- norm_gain: float32 [2048], replicated, may hold values from 0.1 to 1.9
- w_gate: bfloat16 [2048, 5632], P('sp', 'tp'), may hold values from -0.125 to 0.125
- w_up: bfloat16 [2048, 5632], P('sp', 'tp'), may hold values from -0.125 to 0.125
- w_down: bfloat16 [5632, 2048], P('tp', 'sp'), may hold values from -0.078125 to 0.078125
Outputs:
- layer_out: bfloat16 [4096, 2048], P(('sp', 'tp'))
The draws below stay inside these ranges and needn't reach their ends.
Inputs may be any that keep to these rules, and one draw needn't show every extreme that they name: `doc_ids`: document numbers never fall along the sequence; each document covers at most 2048 positions and one covers exactly that many.
All inputs are finite; a program needn't handle non-finite values.
Results may differ from the reference program's by a relative error of at most 0.015.
Values may be sent and summed in bfloat16 or wider, within the bound.
A program may use at most 64 MiB of HBM per device.

```python
import math
import jax
import jax.numpy as jnp
import numpy as np
from jax import lax

D = 2048
HEADS = 16
KV_HEADS = 8
HEAD = 64
FF = 5632
WINDOW = 128
TOK_DEV = 512
TOKENS = 4096
DOCS = 4
DOC_MOST = 2048
N_SP = 8
N_TP = 4


def draw_k_proj(key, part):
    base = jnp.clip(jax.random.normal(jax.random.fold_in(key, 3), (TOKENS, KV_HEADS * HEAD), jnp.float32), -5.0, 5.0)
    return base.astype(jnp.bfloat16)


def draw_q_proj(key, part):
    base = jnp.clip(jax.random.normal(jax.random.fold_in(key, 5), (TOKENS, HEADS * HEAD), jnp.float32), -5.0, 5.0)
    return base.astype(jnp.bfloat16)


def draw_resid(key, part):
    block_total = D // 32
    scales = jnp.exp(jax.random.uniform(jax.random.fold_in(key, 21), (block_total,), jnp.float32, math.log(0.3), math.log(3.0)))
    column_scales = jnp.repeat(scales, 32)
    base = jnp.clip(jax.random.normal(jax.random.fold_in(key, 23), (TOKENS, D), jnp.float32), -4.0, 4.0)
    return (base * column_scales[None, :]).astype(jnp.bfloat16)


def block_scale(own_key, dims, shards, low, largest):
    level, own = 1.0, jax.random.fold_in(own_key, 6)
    for position, shards_of in shards:
        steps = jnp.exp(jax.random.uniform(jax.random.fold_in(own, position), (shards_of,), jnp.float32, low / len(shards), largest / len(shards)))
        level = level * jnp.repeat(steps, dims[position] // shards_of).reshape([-1 if axis == position else 1 for axis in range(len(dims))])
    return level


def split_up(amount, total, most, slope):
    loads = [(1 << 20) // math.isqrt(standing ** slope) + 1 for standing in range(2, amount + 1)]
    surplus, holding = total - most - (amount - 1), [1] * (amount - 1)
    while surplus > 0:
        candidates = [i for i in range(amount - 1) if holding[i] < most]
        mass, remaining = sum([loads[i] for i in candidates]), surplus
        for i in candidates:
            addition = min(most - holding[i], max(1, remaining * loads[i] // mass), surplus)
            holding[i] = holding[i] + addition
            surplus = surplus - addition
    return np.array([most] + holding)


def ragged(own_key, number_of, total, most, slope):
    if number_of == 2:
        one = jax.random.randint(own_key, (), max(1, total - most), min(most, total - 1) + 1)
        return jnp.stack([one, total - one])
    lengths = jnp.asarray(split_up(number_of, total, most, slope), jnp.int32)
    couples = (number_of - 1) // 2
    donor, taker = lengths[1:1 + 2 * couples:2], lengths[2:2 + 2 * couples:2]
    margin = jnp.minimum(donor - 1, most - taker)
    shifted = jax.random.randint(jax.random.fold_in(own_key, 1), (couples,), 0, 1 << 20) % (margin + 1)
    lengths = lengths.at[1:1 + 2 * couples:2].set(donor - shifted).at[2:2 + 2 * couples:2].set(taker + shifted)
    return lengths[jax.random.permutation(jax.random.fold_in(own_key, 2), number_of)]


def gaussian(own_key, dims, deviation, bound, shards=(), held_as=jnp.bfloat16):
    entries = jax.random.normal(own_key, dims, jnp.float32) * deviation
    if len(shards) > 0:
        entries = block_scale(own_key, dims, shards, -0.22, 0.18) * entries
    return jnp.clip(entries, min=-bound, max=bound).astype(held_as)


def setup_inputs(seed: int = 0) -> dict:
    key_list = jax.random.split(jax.random.key(seed), 12)
    q_proj = draw_q_proj(jax.random.fold_in(key_list[11], 71), 0)
    k_proj = draw_k_proj(jax.random.fold_in(key_list[11], 71), 0)
    v_proj = gaussian(key_list[2], (TOKENS, KV_HEADS * HEAD), 1.0, 6.0, ((0, 8), (1, 4)))
    doc_ids = jnp.searchsorted(jnp.cumsum(ragged(key_list[3], DOCS, TOKENS, DOC_MOST, 2)), jnp.arange(TOKENS), side="right").astype(jnp.int32)
    sinks = jnp.clip(0.5 + 5.0 * jax.random.uniform(key_list[4], (HEADS,), jnp.float32) ** block_scale(key_list[4], (HEADS,), ((0, 4),), -0.2, 0.2), 0.5, 5.5)
    resid = draw_resid(jax.random.fold_in(key_list[11], 71), 0)
    w_out = gaussian(key_list[6], (HEADS * HEAD, D), 0.25, 4.0, ((0, 4),))
    norm_gain = jnp.clip(1.0 + 0.18 * jax.random.normal(key_list[7], (D,), jnp.float32), 0.1, 1.9)
    w_gate = gaussian(key_list[8], (D, FF), D ** -0.5, 0.125, ((0, 8), (1, 4)))
    w_up = gaussian(key_list[9], (D, FF), D ** -0.5, 0.125, ((0, 8), (1, 4)))
    w_down = gaussian(key_list[10], (FF, D), FF ** -0.5, 0.078125, ((0, 4), (1, 8)))
    return {"q_proj": q_proj, "k_proj": k_proj, "v_proj": v_proj, "doc_ids": doc_ids, "sinks": sinks, "resid": resid, "w_out": w_out, "norm_gain": norm_gain, "w_gate": w_gate, "w_up": w_up, "w_down": w_down}


norm_eps = 1e-06
masked = -1e+30

def reference(q_proj, k_proj, v_proj, doc_ids, sinks, resid, w_out, norm_gain, w_gate, w_up, w_down):
    groups = HEADS // KV_HEADS
    block_count = TOKENS // WINDOW
    scale = HEAD ** (-0.5)
    padding = jnp.zeros((WINDOW, KV_HEADS * HEAD), jnp.bfloat16)
    keys_pad = jnp.concatenate([padding, k_proj, padding], axis=0)
    values_pad = jnp.concatenate([padding, v_proj, padding], axis=0)
    edge_docs = jnp.full((WINDOW,), -1, jnp.int32)
    docs_pad = jnp.concatenate([edge_docs, doc_ids.astype(jnp.int32), edge_docs], axis=0)
    offsets = jnp.arange(3 * WINDOW, dtype=jnp.int32) - WINDOW
    near = jnp.abs(jnp.arange(WINDOW, dtype=jnp.int32)[:, None] - offsets[None, :]) <= WINDOW
    sink_table = sinks.reshape(KV_HEADS, groups)[:, :, None, None]

    def attend_block(index):
        first = (index * WINDOW).astype(jnp.int32)
        queries = lax.dynamic_slice_in_dim(q_proj, first, WINDOW, 0).astype(jnp.float32).reshape(WINDOW, KV_HEADS, groups, HEAD)
        keys = lax.dynamic_slice_in_dim(keys_pad, first, 3 * WINDOW, 0).astype(jnp.float32).reshape(3 * WINDOW, KV_HEADS, HEAD)
        values = lax.dynamic_slice_in_dim(values_pad, first, 3 * WINDOW, 0).astype(jnp.float32).reshape(3 * WINDOW, KV_HEADS, HEAD)
        key_docs = lax.dynamic_slice_in_dim(docs_pad, first, 3 * WINDOW, 0)
        query_docs = lax.dynamic_slice_in_dim(doc_ids.astype(jnp.int32), first, WINDOW, 0)
        valid = near & (query_docs[:, None] == key_docs[None, :])
        scores = jnp.einsum('qhgd,khd->hgqk', queries, keys) * scale
        scores = jnp.where(valid[None, None], scores, masked)
        top = jnp.maximum(lax.optimization_barrier(jnp.max(scores, axis=-1, keepdims=True)), sink_table)
        expd = jnp.exp(scores - top)
        probs = (expd / (lax.optimization_barrier(jnp.sum(expd, axis=-1, keepdims=True)) + jnp.exp(sink_table - top))).astype(jnp.bfloat16)
        mixed = jnp.einsum('hgqk,khd->qhgd', probs.astype(jnp.float32), values)
        return mixed.reshape(WINDOW, HEADS * HEAD).astype(jnp.bfloat16)
    attended = lax.map(attend_block, jnp.arange(block_count, dtype=jnp.int32)).reshape(TOKENS, HEADS * HEAD)
    mixer_sum = jnp.dot(attended, w_out, preferred_element_type=jnp.float32)
    middle = resid.astype(jnp.float32) + mixer_sum
    normed = (middle * lax.rsqrt(lax.optimization_barrier(jnp.mean(middle * middle, axis=-1, keepdims=True)) + norm_eps) * norm_gain).astype(jnp.bfloat16)
    ffn_width = FF // N_TP

    def ffn_block(block_rows):
        gate = jnp.dot(block_rows, w_gate, preferred_element_type=jnp.float32)
        up_part = jnp.dot(block_rows, w_up, preferred_element_type=jnp.float32)
        hidden = (jax.nn.silu(gate) * up_part).astype(jnp.bfloat16)
        total = jnp.zeros((block_rows.shape[0], D), jnp.float32)
        for group in range(N_TP):
            lower = group * ffn_width
            partial_down = jnp.dot(hidden[:, lower:lower + ffn_width], w_down[lower:lower + ffn_width], preferred_element_type=jnp.float32).astype(jnp.bfloat16)
            total = total + lax.optimization_barrier(partial_down).astype(jnp.float32)
        return total
    ffn_sum = lax.map(ffn_block, normed.reshape(N_SP, TOK_DEV, D)).reshape(TOKENS, D)
    return (middle + ffn_sum).astype(jnp.bfloat16)
```

```python
import functools

import jax
import jax.numpy as jnp
from jax import lax
from jax.experimental import pallas as pl
from jax.experimental.pallas import tpu as pltpu
from jax.sharding import PartitionSpec as P

HEAD = 64
WINDOW = 128
norm_eps = 1e-06
masked = -1e30
MESH = pl.DeviceIdType.MESH


def kernel(
    Z, Y, T,
    q_ref, k_ref, v_ref, drow_ref, dcol_ref, sink_ref, resid_ref, gain_ref, wo_hbm, wg_hbm, wu_hbm, wd_hbm,
    out_ref,
    G, U, D, kext, vext, dext, att, rows, WO, mid, NB, gacc, uacc, hid, PT, RT,
    loc_sem, halo_s, halo_r, wo_s, wo_r, at_s, at_r, nb_s, nb_r, pt_s, pt_r, w_s, w_r, b_s,
):
    n_sp = Z * Y
    s, t = lax.axis_index("sp"), lax.axis_index("tp")
    z, y = s // Y, s % Y
    tok = q_ref.shape[0]
    nb = tok // WINDOW
    own = tok // T
    heads = q_ref.shape[1] // HEAD
    groups = heads // (k_ref.shape[1] // HEAD)
    kb = G.shape[1]
    ff = G.shape[2]
    half = D.shape[1] // 2
    mats = (G, U, D.at[:, half:], D.at[:, :half])

    def rcopy(src, dst, ssem, rsem, sp_to, tp_to):
        return pltpu.make_async_remote_copy(
            src_ref=src, dst_ref=dst, send_sem=ssem, recv_sem=rsem,
            device_id={"sp": sp_to, "tp": tp_to}, device_id_type=MESH,
        )

    def arrived(ref, sem):
        pltpu.make_async_copy(ref, ref, sem).wait()

    def piece(m, slot):
        if m < 2:
            return (G, U)[m].at[slot]
        return D.at[slot, pl.ds(half if m == 2 else 0, half)]

    locals_ = [
        pltpu.make_async_copy(wd_hbm, D.at[s], loc_sem.at[2]),
        pltpu.make_async_copy(wg_hbm, G.at[s], loc_sem.at[0]),
        pltpu.make_async_copy(wu_hbm, U.at[s], loc_sem.at[1]),
        pltpu.make_async_copy(wo_hbm, WO.at[t], loc_sem.at[3]),
    ]
    for c in locals_:
        c.start()

    right, left = (s + 1) % n_sp, (s + n_sp - 1) % n_sp
    halos = []
    for i, (src, dst) in enumerate(((k_ref, kext), (v_ref, vext))):
        halos.append((src.at[pl.ds(tok - WINDOW, WINDOW)], dst.at[pl.ds(0, WINDOW)], 2 * i, right))
        halos.append((src.at[pl.ds(0, WINDOW)], dst.at[pl.ds(tok + WINDOW, WINDOW)], 2 * i + 1, left))
    halos.append((drow_ref.at[nb - 1], dext.at[0], 4, right))
    halos.append((drow_ref.at[0], dext.at[nb + 1], 5, left))
    halo_copies = [rcopy(a, b, halo_s.at[i], halo_r.at[i], to, t) for a, b, i, to in halos]
    for c in halo_copies:
        c.start()

    def up_copy(m, slot, sem):
        return rcopy(piece(m, slot), piece(m, slot), sem, w_r.at[m, slot], s + Y, t)

    def down_copy(m, slot, sem):
        return rcopy(piece(m, slot), piece(m, slot), sem, w_r.at[m, slot], s - Y, t)

    def z_sem(m, way, zz, yy):
        return b_s.at[way, zz * Y + yy] if m == 3 else w_s.at[m, way, zz]

    def send_up(m, zz, yy):
        @pl.when(z + 1 < Z)
        def _():
            up_copy(m, zz * Y + yy, z_sem(m, 0, zz, yy)).start()

    def send_down(m, zz, yy):
        @pl.when(z > 0)
        def _():
            down_copy(m, zz * Y + yy, z_sem(m, 1, zz, yy)).start()

    def y_copies(m, zz):
        slot = zz * Y + y
        return [
            rcopy(piece(m, slot), piece(m, slot), w_s.at[m, 1 + j, zz], w_r.at[m, slot], z * Y + (y + j) % Y, t)
            for j in range(1, Y)
        ]

    def send_y(m, zz):
        for c in y_copies(m, zz):
            c.start()

    def tp_peers():
        return [(t + j) % T for j in range(1, T)]

    for c in locals_[:1]:
        c.wait()
    send_y(3, z)
    for m in (0, 1):
        locals_[1 + m].wait()
        send_up(m, z, y)
        send_down(m, z, y)
        send_y(m, z)
    locals_[3].wait()
    wo_copies = [rcopy(WO.at[t], WO.at[t], wo_s.at[j], wo_r.at[t], s, p) for j, p in enumerate(tp_peers())]
    for c in wo_copies:
        c.start()

    kext[pl.ds(WINDOW, tok)] = k_ref[...]
    vext[pl.ds(WINDOW, tok)] = v_ref[...]
    dext[pl.ds(1, nb)] = drow_ref[...]
    for a, b, i, to in halos:
        arrived(b, halo_r.at[i])
    row_at = lax.broadcasted_iota(jnp.int32, (WINDOW, 3 * WINDOW), 0)
    col_at = lax.broadcasted_iota(jnp.int32, (WINDOW, 3 * WINDOW), 1) - WINDOW
    near = jnp.abs(row_at - col_at) <= WINDOW

    @pl.loop(0, nb)
    def _(blk):
        base = pl.multiple_of(blk * WINDOW, WINDOW)
        place = s * tok + base + col_at
        key_docs = jnp.concatenate([dext[blk + i][0:1] for i in range(3)], axis=1)
        query_docs = dcol_ref[pl.ds(base, WINDOW), 0:1]
        valid = near & (place >= 0) & (place < tok * n_sp) & (query_docs == key_docs)
        qs = q_ref[pl.ds(base, WINDOW)]
        ks = kext[pl.ds(base, 3 * WINDOW)]
        vs = vext[pl.ds(base, 3 * WINDOW)]
        outs = []
        for h in range(heads):
            g = h // groups
            scores = lax.dot_general(
                qs[:, h * HEAD:(h + 1) * HEAD], ks[:, g * HEAD:(g + 1) * HEAD],
                (((1,), (1,)), ((), ())), preferred_element_type=jnp.float32,
            ) * HEAD ** (-0.5)
            scores = jnp.where(valid, scores, masked)
            sink = sink_ref[h]
            top = jnp.maximum(jnp.max(scores, axis=-1, keepdims=True), sink)
            expd = jnp.exp(scores - top)
            total = jnp.sum(expd, axis=-1, keepdims=True) + jnp.exp(sink - top)
            probs = (expd / total).astype(jnp.bfloat16)
            outs.append(jnp.dot(probs, vs[:, g * HEAD:(g + 1) * HEAD], preferred_element_type=jnp.float32))
        att[pl.ds(base, WINDOW)] = jnp.concatenate(outs, axis=1).astype(jnp.bfloat16)

    at_copies = [
        rcopy(att.at[pl.ds(pl.multiple_of(p * own, own), own)], rows.at[t], at_s.at[j], at_r.at[t], s, p)
        for j, p in enumerate(tp_peers())
    ]
    for c in at_copies:
        c.start()
    rows[t] = att[pl.ds(pl.multiple_of(t * own, own), own)]

    def handle(ms, r):
        for m in ms:
            for sign in (-1, 1):
                zz = z + sign * r

                @pl.when((zz >= 0) & (zz < Z))
                def _():
                    send = send_up if sign < 0 else send_down
                    columns = range(Y) if m == 3 else (0,)
                    for j in columns:
                        yy = (y + j) % Y
                        arrived(piece(m, zz * Y + yy), w_r.at[m, zz * Y + yy])
                        send(m, zz, yy)
                    if m != 3:
                        send_y(m, zz)

    def project():
        for p in tp_peers():
            arrived(WO.at[p], wo_r.at[p])
            arrived(rows.at[p], at_r.at[p])
        middle = resid_ref[...].astype(jnp.float32)
        for i in range(T):
            middle = middle + jnp.dot(rows[i], WO[i], preferred_element_type=jnp.float32)
        mid[...] = middle
        normed = (
            middle * lax.rsqrt(jnp.mean(middle * middle, axis=-1, keepdims=True) + norm_eps) * gain_ref[...]
        ).astype(jnp.bfloat16)
        mine = pl.ds(pl.multiple_of(t * own, own), own)
        for i in range(n_sp):
            NB[i, mine] = normed[:, i * kb:(i + 1) * kb]
        for c in nb_copies():
            c.start()

    def nb_rows(p):
        return NB.at[:, pl.ds(pl.multiple_of(p * own, own), own)]

    def nb_copies():
        return [rcopy(nb_rows(t), nb_rows(t), nb_s.at[j], nb_r.at[t], s, p) for j, p in enumerate(tp_peers())]

    step = min(tok, 256)

    def each(r, body):
        @pl.loop(0, (2 if r else 1) * Y)
        def _(i):
            joff = i % Y
            zz = z + (2 * (i // Y) - 1) * r
            slot = zz * Y + (y + joff) % Y

            @pl.when((zz >= 0) & (zz < Z))
            def _():
                body(slot, joff)

    def gate_up(r):
        def body(slot, joff):
            @pl.when(joff > 0)
            def _():
                for m in (0, 1):
                    arrived(piece(m, slot), w_r.at[m, slot])

            @pl.loop(0, tok // step)
            def _(i):
                at = pl.ds(pl.multiple_of(i * step, step), step)
                x = NB[slot, at]
                gacc[at] += jnp.dot(x, G[slot], preferred_element_type=jnp.float32)
                uacc[at] += jnp.dot(x, U[slot], preferred_element_type=jnp.float32)

        each(r, body)

    def pt_rows(slot, p):
        return PT.at[slot, pl.ds(pl.multiple_of(p * own, own), own)]

    def down(r):
        def body(slot, joff):
            @pl.when(joff > 0)
            def _():
                arrived(piece(2, slot), w_r.at[2, slot])

            @pl.loop(0, tok // step)
            def _(i):
                at = pl.ds(pl.multiple_of(i * step, step), step)
                PT[slot, at] = jnp.dot(hid[at], D[slot], preferred_element_type=jnp.float32).astype(jnp.bfloat16)

            for j, p in enumerate(tp_peers()):
                rcopy(pt_rows(slot, p), RT.at[t, slot], pt_s.at[j], pt_r.at[t], s, p).start()

        each(r, body)

    gacc[...] = jnp.zeros_like(gacc)
    uacc[...] = jnp.zeros_like(uacc)
    if Z > 1:
        handle((0, 1), 1)
    project()
    if Z > 2:
        handle((0, 1), 2)
    for p in tp_peers():
        arrived(nb_rows(p), nb_r.at[p])
    gate_up(0)
    for r in range(3, Z):
        handle((0, 1), r)
        gate_up(r - 2)

    for j in range(1, Y):
        slot = z * Y + (y + j) % Y
        arrived(piece(3, slot), w_r.at[3, slot])
    send_up(2, z, y)
    send_down(2, z, y)
    send_y(2, z)
    for j in range(Y):
        send_up(3, z, (y + j) % Y)
        send_down(3, z, (y + j) % Y)
    for r in range(max(1, Z - 2), Z - 1):
        gate_up(r)
    if Z > 1:
        handle((2, 3), 1)
        gate_up(Z - 1)

    @pl.loop(0, tok // WINDOW)
    def _(i):
        at = pl.ds(pl.multiple_of(i * WINDOW, WINDOW), WINDOW)
        gate = gacc[at]
        hid[at] = (gate / (1.0 + jnp.exp(-gate)) * uacc[at]).astype(jnp.bfloat16)

    down(0)
    for r in range(1, Z):
        if r + 1 < Z:
            handle((2, 3), r + 1)
        down(r)

    for p in tp_peers():
        arrived(RT.at[p], pt_r.at[p])
    for i in range(n_sp):
        cols = slice(i * kb, (i + 1) * kb)
        total = mid[:, cols] + PT[i, pl.ds(pl.multiple_of(t * own, own), own)].astype(jnp.float32)
        for p in tp_peers():
            total = total + RT[p, i].astype(jnp.float32)
        out_ref[:, cols] = total.astype(jnp.bfloat16)

    for c in halo_copies + wo_copies + at_copies + nb_copies():
        c.wait_send()
    for j, p in enumerate(tp_peers()):
        arrived(PT.at[:, pl.ds(pl.multiple_of(p * own, own), own)], pt_s.at[j])
    for c in y_copies(3, z):
        c.wait_send()
    for zz in range(Z):
        for m in range(3):
            for c in y_copies(m, zz):
                c.wait_send()
        for m in range(4):
            for j in range(Y if m == 3 else 1):
                yy = (y + j) % Y

                @pl.when((zz <= z) & (z + 1 < Z))
                def _():
                    up_copy(m, zz * Y + yy, z_sem(m, 0, zz, yy)).wait_send()

                @pl.when((zz >= z) & (z > 0))
                def _():
                    down_copy(m, zz * Y + yy, z_sem(m, 1, zz, yy)).wait_send()


def shards(Z, Y, T, q, k, v, doc_ids, sinks, resid, w_out, gain, wg, wu, wd):
    n_sp = Z * Y
    tok, (kb, ff), d = q.shape[0], wg.shape, resid.shape[1]
    nb, own = tok // WINDOW, tok // T
    bf, f32 = jnp.bfloat16, jnp.float32
    drow = jnp.broadcast_to(doc_ids.reshape(nb, 1, WINDOW), (nb, 8, WINDOW))
    dcol = jnp.broadcast_to(doc_ids[:, None], (tok, 128))
    vmem, hbm = pl.BlockSpec(memory_space=pltpu.VMEM), pl.BlockSpec(memory_space=pl.ANY)
    dma = pltpu.SemaphoreType.DMA
    V = pltpu.VMEM
    return pl.pallas_call(
        functools.partial(kernel, Z, Y, T),
        out_shape=jax.ShapeDtypeStruct((own, d), bf),
        in_specs=[vmem] * 5 + [pl.BlockSpec(memory_space=pltpu.SMEM)] + [vmem] * 2 + [hbm] * 4,
        out_specs=vmem,
        scratch_shapes=[
            V((n_sp, kb, ff), bf), V((n_sp, kb, ff), bf), V((n_sp, ff, wd.shape[1]), bf),
            V((tok + 2 * WINDOW, k.shape[1]), bf), V((tok + 2 * WINDOW, k.shape[1]), bf),
            V((nb + 2, 8, WINDOW), jnp.int32),
            V((tok, q.shape[1]), bf), V((T, own, q.shape[1]), bf), V((T,) + w_out.shape, bf),
            V((own, d), f32), V((n_sp, tok, kb), bf), V((tok, ff), f32), V((tok, ff), f32), V((tok, ff), bf),
            V((n_sp, tok, kb), bf), V((T, n_sp, own, kb), bf),
            dma((4,)), dma((6,)), dma((6,)),
            dma((T,)), dma((T,)), dma((T,)), dma((T,)), dma((T,)), dma((T,)), dma((T,)), dma((T,)),
            dma((4, 1 + Y, Z)), dma((4, n_sp)), dma((2, n_sp)),
        ],
        compiler_params=pltpu.CompilerParams(has_side_effects=True, vmem_limit_bytes=60 * 1024 * 1024),
    )(q, k, v, drow, dcol, sinks, resid, gain.reshape(1, d), w_out, wg, wu, wd)


def solution(mesh):
    n_sp, T = mesh.shape["sp"], mesh.shape["tp"]
    Y = 2 if n_sp <= 8 else 4
    while n_sp % Y:
        Y //= 2
    placed = (
        P("sp", "tp"),
        P("sp", "tp"),
        P("sp", "tp"),
        P("sp"),
        P("tp"),
        P(("sp", "tp"), None),
        P("tp", None),
        P(),
        P("sp", "tp"),
        P("sp", "tp"),
        P("tp", "sp"),
    )
    return jax.shard_map(
        functools.partial(shards, n_sp // Y, Y, T), mesh=mesh, in_specs=placed,
        out_specs=P(("sp", "tp"), None), check_vma=False,
    )
```

```python
import functools

import jax
import jax.numpy as jnp
from jax import lax
from jax.experimental import pallas as pl
from jax.experimental.pallas import tpu as pltpu
from jax.sharding import PartitionSpec as P

HEAD = 64
WINDOW = 128
norm_eps = 1e-06
masked = -1e30
MESH = pl.DeviceIdType.MESH


def attend(n_sp, s, q_ref, k_ref, v_ref, drow_ref, dcol_ref, sink_ref, kext, vext, dext, att, wait_halo):
    tok = q_ref.shape[0]
    nb = tok // WINDOW
    heads = q_ref.shape[1] // HEAD
    groups = heads // (k_ref.shape[1] // HEAD)
    kext[pl.ds(WINDOW, tok)] = k_ref[...]
    vext[pl.ds(WINDOW, tok)] = v_ref[...]
    dext[pl.ds(1, nb)] = drow_ref[...]
    wait_halo()
    row_at = lax.broadcasted_iota(jnp.int32, (WINDOW, 3 * WINDOW), 0)
    col_at = lax.broadcasted_iota(jnp.int32, (WINDOW, 3 * WINDOW), 1) - WINDOW
    near = jnp.abs(row_at - col_at) <= WINDOW

    @pl.loop(0, nb)
    def _(blk):
        base = pl.multiple_of(blk * WINDOW, WINDOW)
        place = s * tok + base + col_at
        key_docs = jnp.concatenate([dext[blk + i][0:1] for i in range(3)], axis=1)
        query_docs = dcol_ref[pl.ds(base, WINDOW), 0:1]
        valid = near & (place >= 0) & (place < tok * n_sp) & (query_docs == key_docs)
        qs = q_ref[pl.ds(base, WINDOW)]
        ks = kext[pl.ds(base, 3 * WINDOW)]
        vs = vext[pl.ds(base, 3 * WINDOW)]
        outs = []
        for h in range(heads):
            g = h // groups
            scores = lax.dot_general(
                qs[:, h * HEAD:(h + 1) * HEAD], ks[:, g * HEAD:(g + 1) * HEAD],
                (((1,), (1,)), ((), ())), preferred_element_type=jnp.float32,
            ) * HEAD ** (-0.5)
            scores = jnp.where(valid, scores, masked)
            sink = sink_ref[h]
            top = jnp.maximum(jnp.max(scores, axis=-1, keepdims=True), sink)
            expd = jnp.exp(scores - top)
            total = jnp.sum(expd, axis=-1, keepdims=True) + jnp.exp(sink - top)
            probs = (expd / total).astype(jnp.bfloat16)
            outs.append(jnp.dot(probs, vs[:, g * HEAD:(g + 1) * HEAD], preferred_element_type=jnp.float32))
        att[pl.ds(base, WINDOW)] = jnp.concatenate(outs, axis=1).astype(jnp.bfloat16)


def kernel(
    Z, Y, T,
    q_ref, k_ref, v_ref, drow_ref, dcol_ref, sink_ref, resid_ref, gain_ref, wo_hbm, wg_hbm, wu_hbm, wd_hbm,
    out_ref,
    G, U, D, kext, vext, dext, att, rows, WO, mid, NB, gacc, uacc, hid, PT, RT,
    loc_sem, halo_s, halo_r, wo_s, wo_r, at_s, at_r, nb_s, nb_r, pt_s, pt_r, w_s, w_r, b_s,
):
    n_sp = Z * Y
    s, t = lax.axis_index("sp"), lax.axis_index("tp")
    z, y = s // Y, s % Y
    tok = q_ref.shape[0]
    nb = tok // WINDOW
    own = tok // T
    kb = G.shape[1]
    half = D.shape[1] // 2

    def rcopy(src, dst, ssem, rsem, sp_to, tp_to):
        return pltpu.make_async_remote_copy(
            src_ref=src, dst_ref=dst, send_sem=ssem, recv_sem=rsem,
            device_id={"sp": sp_to, "tp": tp_to}, device_id_type=MESH,
        )

    def arrived(ref, sem):
        pltpu.make_async_copy(ref, ref, sem).wait()

    def piece(m, slot):
        if m < 2:
            return (G, U)[m].at[slot]
        return D.at[slot, pl.ds(half if m == 2 else 0, half)]

    locals_ = [
        pltpu.make_async_copy(wd_hbm, D.at[s], loc_sem.at[2]),
        pltpu.make_async_copy(wg_hbm, G.at[s], loc_sem.at[0]),
        pltpu.make_async_copy(wu_hbm, U.at[s], loc_sem.at[1]),
        pltpu.make_async_copy(wo_hbm, WO.at[t], loc_sem.at[3]),
    ]
    for c in locals_:
        c.start()

    right, left = (s + 1) % n_sp, (s + n_sp - 1) % n_sp
    halos = []
    for i, (src, dst) in enumerate(((k_ref, kext), (v_ref, vext))):
        halos.append((src.at[pl.ds(tok - WINDOW, WINDOW)], dst.at[pl.ds(0, WINDOW)], 2 * i, right))
        halos.append((src.at[pl.ds(0, WINDOW)], dst.at[pl.ds(tok + WINDOW, WINDOW)], 2 * i + 1, left))
    halos.append((drow_ref.at[nb - 1], dext.at[0], 4, right))
    halos.append((drow_ref.at[0], dext.at[nb + 1], 5, left))
    halo_copies = [rcopy(a, b, halo_s.at[i], halo_r.at[i], to, t) for a, b, i, to in halos]
    for c in halo_copies:
        c.start()

    def up_copy(m, slot, sem):
        return rcopy(piece(m, slot), piece(m, slot), sem, w_r.at[m, slot], s + Y, t)

    def down_copy(m, slot, sem):
        return rcopy(piece(m, slot), piece(m, slot), sem, w_r.at[m, slot], s - Y, t)

    def z_sem(m, way, zz, yy):
        return b_s.at[way, zz * Y + yy] if m == 3 else w_s.at[m, way, zz]

    def send_up(m, zz, yy):
        @pl.when(z + 1 < Z)
        def _():
            up_copy(m, zz * Y + yy, z_sem(m, 0, zz, yy)).start()

    def send_down(m, zz, yy):
        @pl.when(z > 0)
        def _():
            down_copy(m, zz * Y + yy, z_sem(m, 1, zz, yy)).start()

    def y_copies(m, zz):
        slot = zz * Y + y
        return [
            rcopy(piece(m, slot), piece(m, slot), w_s.at[m, 1 + j, zz], w_r.at[m, slot], z * Y + (y + j) % Y, t)
            for j in range(1, Y)
        ]

    def send_y(m, zz):
        for c in y_copies(m, zz):
            c.start()

    def tp_peers():
        return [(t + j) % T for j in range(1, T)]

    for c in locals_[:1]:
        c.wait()
    send_y(3, z)
    for m in (0, 1):
        locals_[1 + m].wait()
        send_up(m, z, y)
        send_down(m, z, y)
        send_y(m, z)
    locals_[3].wait()
    wo_copies = [rcopy(WO.at[t], WO.at[t], wo_s.at[j], wo_r.at[t], s, p) for j, p in enumerate(tp_peers())]
    for c in wo_copies:
        c.start()

    attend(
        n_sp, s, q_ref, k_ref, v_ref, drow_ref, dcol_ref, sink_ref, kext, vext, dext, att,
        lambda: [arrived(b, halo_r.at[i]) for a, b, i, to in halos],
    )

    at_copies = [
        rcopy(att.at[pl.ds(pl.multiple_of(p * own, own), own)], rows.at[t], at_s.at[j], at_r.at[t], s, p)
        for j, p in enumerate(tp_peers())
    ]
    for c in at_copies:
        c.start()
    rows[t] = att[pl.ds(pl.multiple_of(t * own, own), own)]

    def handle(ms, r):
        for m in ms:
            for sign in (-1, 1):
                zz = z + sign * r

                @pl.when((zz >= 0) & (zz < Z))
                def _():
                    send = send_up if sign < 0 else send_down
                    columns = range(Y) if m == 3 else (0,)
                    for j in columns:
                        yy = (y + j) % Y
                        arrived(piece(m, zz * Y + yy), w_r.at[m, zz * Y + yy])
                        send(m, zz, yy)
                    if m != 3:
                        send_y(m, zz)

    def project():
        for p in tp_peers():
            arrived(WO.at[p], wo_r.at[p])
            arrived(rows.at[p], at_r.at[p])
        middle = resid_ref[...].astype(jnp.float32)
        for i in range(T):
            middle = middle + jnp.dot(rows[i], WO[i], preferred_element_type=jnp.float32)
        mid[...] = middle
        normed = (
            middle * lax.rsqrt(jnp.mean(middle * middle, axis=-1, keepdims=True) + norm_eps) * gain_ref[...]
        ).astype(jnp.bfloat16)
        mine = pl.ds(pl.multiple_of(t * own, own), own)
        for i in range(n_sp):
            NB[i, mine] = normed[:, i * kb:(i + 1) * kb]
        for c in nb_copies():
            c.start()

    def nb_rows(p):
        return NB.at[:, pl.ds(pl.multiple_of(p * own, own), own)]

    def nb_copies():
        return [rcopy(nb_rows(t), nb_rows(t), nb_s.at[j], nb_r.at[t], s, p) for j, p in enumerate(tp_peers())]

    step = min(tok, 256)

    def each(r, body):
        @pl.loop(0, (2 if r else 1) * Y)
        def _(i):
            joff = i % Y
            zz = z + (2 * (i // Y) - 1) * r
            slot = zz * Y + (y + joff) % Y

            @pl.when((zz >= 0) & (zz < Z))
            def _():
                body(slot, joff)

    def gate_up(r):
        def body(slot, joff):
            @pl.when(joff > 0)
            def _():
                for m in (0, 1):
                    arrived(piece(m, slot), w_r.at[m, slot])

            @pl.loop(0, tok // step)
            def _(i):
                at = pl.ds(pl.multiple_of(i * step, step), step)
                x = NB[slot, at]
                gacc[at] += jnp.dot(x, G[slot], preferred_element_type=jnp.float32)
                uacc[at] += jnp.dot(x, U[slot], preferred_element_type=jnp.float32)

        each(r, body)

    def pt_rows(slot, p):
        return PT.at[slot, pl.ds(pl.multiple_of(p * own, own), own)]

    def down(r):
        def body(slot, joff):
            @pl.when(joff > 0)
            def _():
                arrived(piece(2, slot), w_r.at[2, slot])

            @pl.loop(0, tok // step)
            def _(i):
                at = pl.ds(pl.multiple_of(i * step, step), step)
                PT[slot, at] = jnp.dot(hid[at], D[slot], preferred_element_type=jnp.float32).astype(jnp.bfloat16)

            for j, p in enumerate(tp_peers()):
                rcopy(pt_rows(slot, p), RT.at[t, slot], pt_s.at[j], pt_r.at[t], s, p).start()

        each(r, body)

    gacc[...] = jnp.zeros_like(gacc)
    uacc[...] = jnp.zeros_like(uacc)
    if Z > 1:
        handle((0, 1), 1)
    project()
    if Z > 2:
        handle((0, 1), 2)
    for p in tp_peers():
        arrived(nb_rows(p), nb_r.at[p])
    gate_up(0)
    for r in range(3, Z):
        handle((0, 1), r)
        gate_up(r - 2)

    for j in range(1, Y):
        slot = z * Y + (y + j) % Y
        arrived(piece(3, slot), w_r.at[3, slot])
    send_up(2, z, y)
    send_down(2, z, y)
    send_y(2, z)
    for j in range(Y):
        send_up(3, z, (y + j) % Y)
        send_down(3, z, (y + j) % Y)
    for r in range(max(1, Z - 2), Z - 1):
        gate_up(r)
    if Z > 1:
        handle((2, 3), 1)
        gate_up(Z - 1)

    @pl.loop(0, tok // WINDOW)
    def _(i):
        at = pl.ds(pl.multiple_of(i * WINDOW, WINDOW), WINDOW)
        gate = gacc[at]
        hid[at] = (gate / (1.0 + jnp.exp(-gate)) * uacc[at]).astype(jnp.bfloat16)

    down(0)
    for r in range(1, Z):
        if r + 1 < Z:
            handle((2, 3), r + 1)
        down(r)

    for p in tp_peers():
        arrived(RT.at[p], pt_r.at[p])
    for i in range(n_sp):
        cols = slice(i * kb, (i + 1) * kb)
        total = mid[:, cols] + PT[i, pl.ds(pl.multiple_of(t * own, own), own)].astype(jnp.float32)
        for p in tp_peers():
            total = total + RT[p, i].astype(jnp.float32)
        out_ref[:, cols] = total.astype(jnp.bfloat16)

    for c in halo_copies + wo_copies + at_copies + nb_copies():
        c.wait_send()
    for j, p in enumerate(tp_peers()):
        arrived(PT.at[:, pl.ds(pl.multiple_of(p * own, own), own)], pt_s.at[j])
    for c in y_copies(3, z):
        c.wait_send()
    for zz in range(Z):
        for m in range(3):
            for c in y_copies(m, zz):
                c.wait_send()
        for m in range(4):
            for j in range(Y if m == 3 else 1):
                yy = (y + j) % Y

                @pl.when((zz <= z) & (z + 1 < Z))
                def _():
                    up_copy(m, zz * Y + yy, z_sem(m, 0, zz, yy)).wait_send()

                @pl.when((zz >= z) & (z > 0))
                def _():
                    down_copy(m, zz * Y + yy, z_sem(m, 1, zz, yy)).wait_send()


def paired_kernel(
    Z, Y, T, W,
    q_ref, k_ref, v_ref, drow_ref, dcol_ref, sink_ref, resid_ref, gain_ref, wo_hbm, wg_hbm, wu_hbm, wd_hbm,
    out_ref,
    G, U, D, kext, vext, dext, att, rows, WO, mid, NB, gacc, uacc, hid, PT, RT, ZS, ZR,
    loc_sem, halo_s, halo_r, wo_s, wo_r, at_s, at_r, nb_s, nb_r, pt_s, pt_r, zs_s, zs_r, z_s, y_s, w_r,
):
    n_sp = Z * Y
    s, t = lax.axis_index("sp"), lax.axis_index("tp")
    z, y, x, core = s // Y, s % Y, t // 2, t % 2
    par = z % 2
    s_pair = (z + 1 - 2 * par) * Y + y
    t_pair = x * 2 + 1 - core
    tok = q_ref.shape[0]
    nb = tok // WINDOW
    own = tok // T
    all_tok = 2 * tok
    kb = G.shape[1]
    half = D.shape[1]
    offset = wg_hbm.shape[1] - W
    sent = []

    def rcopy(src, dst, ssem, rsem, sp_to, tp_to):
        return pltpu.make_async_remote_copy(
            src_ref=src, dst_ref=dst, send_sem=ssem, recv_sem=rsem,
            device_id={"sp": sp_to, "tp": tp_to}, device_id_type=MESH,
        )

    def push(*parts):
        c = rcopy(*parts)
        c.start()
        sent.append(c)

    def arrived(ref, sem):
        pltpu.make_async_copy(ref, ref, sem).wait()

    def source(m, which):
        if m < 2:
            return (wg_hbm, wu_hbm)[m].at[:, pl.ds(pl.multiple_of(which * offset, 128), W)]
        return wd_hbm.at[pl.ds(pl.multiple_of(which * half, 16), half)]

    def piece(m, slot):
        return (G, U, D)[m].at[slot]

    def tp_peers():
        return [(t + j) % T for j in range(1, T)]

    def x_peers():
        return [((x + j) % (T // 2)) * 2 + core for j in range(1, T // 2)]

    right, left = (s + 1) % n_sp, (s + n_sp - 1) % n_sp
    halos = []
    for i, (src, dst) in enumerate(((k_ref, kext), (v_ref, vext))):
        halos.append((src.at[pl.ds(tok - WINDOW, WINDOW)], dst.at[pl.ds(0, WINDOW)], 2 * i, right))
        halos.append((src.at[pl.ds(0, WINDOW)], dst.at[pl.ds(tok + WINDOW, WINDOW)], 2 * i + 1, left))
    halos.append((drow_ref.at[nb - 1], dext.at[0], 4, right))
    halos.append((drow_ref.at[0], dext.at[nb + 1], 5, left))
    for a, b, i, to in halos:
        push(a, b, halo_s.at[i], halo_r.at[i], to, t)

    locals_ = [pltpu.make_async_copy(source(m, par), piece(m, s), loc_sem.at[m]) for m in range(3)]
    locals_.append(pltpu.make_async_copy(wo_hbm, WO.at[t], loc_sem.at[3]))
    for c in locals_:
        c.start()

    def z_copy(m, zz):
        return rcopy(source(m, zz % 2), piece(m, s), z_s.at[m, zz], w_r.at[m, s], zz * Y + y, t)

    def send_z(m, r):
        for sign in (-1, 1):
            zz = z + sign * r

            @pl.when((zz >= 0) & (zz < Z))
            def _():
                z_copy(m, zz).start()

    def y_copies(m, zz):
        slot = zz * Y + y
        return [
            rcopy(piece(m, slot), piece(m, slot), y_s.at[m, j, zz], w_r.at[m, slot], z * Y + (y + j) % Y, t)
            for j in range(1, Y)
        ]

    def send_y(m, zz):
        for c in y_copies(m, zz):
            c.start()

    def handle(ms, r):
        for m in ms:
            for sign in (-1, 1):
                zz = z + sign * r

                @pl.when((zz >= 0) & (zz < Z))
                def _():
                    arrived(piece(m, zz * Y + y), w_r.at[m, zz * Y + y])
                    send_y(m, zz)

    for r in range(1, Z):
        for m in (0, 1):
            send_z(m, r)
    for m in (0, 1):
        locals_[m].wait()
        send_y(m, z)
    locals_[2].wait()
    locals_[3].wait()
    for j, p in enumerate(x_peers() + [t_pair]):
        push(WO.at[t], WO.at[t], wo_s.at[j], wo_r.at[t], s, p)

    attend(
        Z * Y, s, q_ref, k_ref, v_ref, drow_ref, dcol_ref, sink_ref, kext, vext, dext, att,
        lambda: [arrived(b, halo_r.at[i]) for a, b, i, to in halos],
    )
    for j, p in enumerate(tp_peers()):
        push(att.at[pl.ds(pl.multiple_of(p * own, own), own)], rows.at[t], at_s.at[j], at_r.at[t], s, p)
    rows[t] = att[pl.ds(pl.multiple_of(t * own, own), own)]

    handle((0, 1), 1)

    for j, p in enumerate(x_peers()):
        arrived(WO.at[p], wo_r.at[p])
        push(WO.at[p], WO.at[p], wo_s.at[T // 2 + j], wo_r.at[p], s, t_pair)
    for p in [t_pair] + [(p // 2) * 2 + 1 - core for p in x_peers()]:
        arrived(WO.at[p], wo_r.at[p])
    for p in tp_peers():
        arrived(rows.at[p], at_r.at[p])
    middle = resid_ref[...].astype(jnp.float32)
    for i in range(T):
        middle = middle + jnp.dot(rows[i], WO[i], preferred_element_type=jnp.float32)
    mid[...] = middle
    normed = (
        middle * lax.rsqrt(jnp.mean(middle * middle, axis=-1, keepdims=True) + norm_eps) * gain_ref[...]
    ).astype(jnp.bfloat16)

    def at_rows(p, which):
        return pl.ds(pl.multiple_of((p * 2 + which) * own, own), own)

    for i in range(n_sp):
        NB[i, at_rows(t, par)] = normed[:, i * kb:(i + 1) * kb]

    def push_rows(p, which, k, sp_to, tp_to):
        part = NB.at[:, at_rows(p, which)]
        push(part, part, nb_s.at[k], nb_r.at[p, which], sp_to, tp_to)

    def wait_rows(p, which):
        arrived(NB.at[:, at_rows(p, which)], nb_r.at[p, which])

    n_x = T // 2
    push_rows(t, par, 0, s_pair, t)
    for j, p in enumerate(x_peers() + [t_pair]):
        push_rows(t, par, 1 + j, s, p)
    for r in range(1, Z):
        send_z(2, r)
    for r in range(2, max(3, Z - 1)):
        if r < Z:
            handle((0, 1), r)
    wait_rows(t, 1 - par)
    for j, p in enumerate(x_peers() + [t_pair]):
        push_rows(t, 1 - par, 1 + n_x + j, s, p)
    for r in range(max(3, Z - 1), Z):
        handle((0, 1), r)
    send_y(2, z)
    for j, p in enumerate(x_peers()):
        for i, which in enumerate((par, 1 - par)):
            wait_rows(p, which)
            push_rows(p, which, 1 + 2 * n_x + 2 * j + i, s, t_pair)
    for p in [t_pair] + [(p // 2) * 2 + 1 - core for p in x_peers()]:
        for which in (par, 1 - par):
            wait_rows(p, which)

    step = min(all_tok, 256)

    def each(r, body):
        @pl.loop(0, (2 if r else 1) * Y)
        def _(i):
            joff = i % Y
            zz = z + (2 * (i // Y) - 1) * r
            slot = zz * Y + (y + joff) % Y

            @pl.when((zz >= 0) & (zz < Z))
            def _():
                body(slot, joff)

    def gate_up(r):
        def body(slot, joff):
            @pl.when(joff > 0)
            def _():
                for m in (0, 1):
                    arrived(piece(m, slot), w_r.at[m, slot])

            @pl.loop(0, all_tok // step)
            def _(i):
                at = pl.ds(pl.multiple_of(i * step, step), step)
                rows_in = NB[slot, at]
                gacc[at] += jnp.dot(rows_in, G[slot], preferred_element_type=jnp.float32)
                uacc[at] += jnp.dot(rows_in, U[slot], preferred_element_type=jnp.float32)

        each(r, body)

    def peer_rows(p):
        return pl.ds(pl.multiple_of(p * 2 * own, 2 * own), 2 * own)

    def down(r):
        def body(slot, joff):
            @pl.when(joff > 0)
            def _():
                arrived(piece(2, slot), w_r.at[2, slot])

            @pl.loop(0, all_tok // step)
            def _(i):
                at = pl.ds(pl.multiple_of(i * step, step), step)
                PT[slot, at] = jnp.dot(hid[at], D[slot], preferred_element_type=jnp.float32).astype(jnp.bfloat16)

            for j, p in enumerate(tp_peers()):
                rcopy(PT.at[slot, peer_rows(p)], RT.at[t, slot], pt_s.at[j], pt_r.at[t, slot], s, p).start()

        each(r, body)

    def reduce(r):
        def body(slot, joff):
            for p in tp_peers():
                arrived(RT.at[p, slot], pt_r.at[p, slot])
            here = pl.ds(pl.multiple_of(par * own, own), own)
            there = pl.ds(pl.multiple_of((1 - par) * own, own), own)
            away = PT[slot, at_rows(t, 1 - par)].astype(jnp.float32)
            for p in tp_peers():
                away = away + RT[p, slot, there].astype(jnp.float32)
            ZS[slot] = away.astype(jnp.bfloat16)
            rcopy(ZS.at[slot], ZR.at[slot], zs_s, zs_r, s_pair, t).start()

        each(r, body)

    gacc[...] = jnp.zeros_like(gacc)
    uacc[...] = jnp.zeros_like(uacc)
    gate_up(0)
    gate_up(1)
    handle((2,), 1)
    for r in range(2, Z):
        gate_up(r)

    @pl.loop(0, all_tok // WINDOW)
    def _(i):
        at = pl.ds(pl.multiple_of(i * WINDOW, WINDOW), WINDOW)
        gate = gacc[at]
        act = (gate / (1.0 + jnp.exp(-gate)) * uacc[at]).astype(jnp.bfloat16)

        @pl.when(par == 0)
        def _():
            hid[at] = act[:, :half]

        @pl.when(par == 1)
        def _():
            hid[at] = act[:, W - half:]

    down(0)
    for r in range(1, Z):
        if r + 1 < Z:
            handle((2,), r + 1)
        down(r)
        reduce(r - 1)
    reduce(Z - 1)

    arrived(ZR, zs_r)
    here = pl.ds(pl.multiple_of(par * own, own), own)
    for i in range(n_sp):
        cols = slice(i * kb, (i + 1) * kb)
        total = mid[:, cols] + PT[i, at_rows(t, par)].astype(jnp.float32) + ZR[i].astype(jnp.float32)
        for p in tp_peers():
            total = total + RT[p, i, here].astype(jnp.float32)
        out_ref[:, cols] = total.astype(jnp.bfloat16)

    for c in sent:
        c.wait_send()
    for j, p in enumerate(tp_peers()):
        arrived(PT.at[:, peer_rows(p)], pt_s.at[j])
    arrived(ZS, zs_s)
    for m in range(3):
        for zz in range(Z):
            for c in y_copies(m, zz):
                c.wait_send()

            @pl.when(z != zz)
            def _():
                z_copy(m, zz).wait_send()


def shards(Z, Y, T, q, k, v, doc_ids, sinks, resid, w_out, gain, wg, wu, wd):
    n_sp = Z * Y
    tok, (kb, ff), d = q.shape[0], wg.shape, resid.shape[1]
    nb, own = tok // WINDOW, tok // T
    bf, f32 = jnp.bfloat16, jnp.float32
    drow = jnp.broadcast_to(doc_ids.reshape(nb, 1, WINDOW), (nb, 8, WINDOW))
    dcol = jnp.broadcast_to(doc_ids[:, None], (tok, 128))
    vmem, hbm = pl.BlockSpec(memory_space=pltpu.VMEM), pl.BlockSpec(memory_space=pl.ANY)
    dma = pltpu.SemaphoreType.DMA
    V = pltpu.VMEM
    specs = [vmem] * 5 + [pl.BlockSpec(memory_space=pltpu.SMEM)] + [vmem] * 2 + [hbm] * 4
    params = pltpu.CompilerParams(has_side_effects=True, vmem_limit_bytes=60 * 1024 * 1024)
    operands = (q, k, v, drow, dcol, sinks, resid, gain.reshape(1, d), w_out, wg, wu, wd)
    half = ff // 2
    W = -(-half // 128) * 128
    if Z % 2 == 0 and T % 2 == 0 and (ff - W) % 128 == 0 and half % 16 == 0 and kb % 128 == 0:
        return pl.pallas_call(
            functools.partial(paired_kernel, Z, Y, T, W),
            out_shape=jax.ShapeDtypeStruct((own, d), bf),
            in_specs=specs,
            out_specs=vmem,
            scratch_shapes=[
                V((n_sp, kb, W), bf), V((n_sp, kb, W), bf), V((n_sp, half, wd.shape[1]), bf),
                V((tok + 2 * WINDOW, k.shape[1]), bf), V((tok + 2 * WINDOW, k.shape[1]), bf),
                V((nb + 2, 8, WINDOW), jnp.int32),
                V((tok, q.shape[1]), bf), V((T, own, q.shape[1]), bf), V((T,) + w_out.shape, bf),
                V((own, d), f32), V((n_sp, 2 * tok, kb), bf),
                V((2 * tok, W), f32), V((2 * tok, W), f32), V((2 * tok, half), bf),
                V((n_sp, 2 * tok, kb), bf), V((T, n_sp, 2 * own, kb), bf),
                V((n_sp, own, kb), bf), V((n_sp, own, kb), bf),
                dma((4,)), dma((6,)), dma((6,)),
                dma((T,)), dma((T,)), dma((T,)), dma((T,)), dma((2 * T + 1,)), dma((T, 2)),
                dma((T,)), dma((T, n_sp)), dma(()), dma(()),
                dma((3, Z)), dma((3, Y, Z)), dma((3, n_sp)),
            ],
            compiler_params=params,
        )(*operands)
    return pl.pallas_call(
        functools.partial(kernel, Z, Y, T),
        out_shape=jax.ShapeDtypeStruct((own, d), bf),
        in_specs=specs,
        out_specs=vmem,
        scratch_shapes=[
            V((n_sp, kb, ff), bf), V((n_sp, kb, ff), bf), V((n_sp, ff, wd.shape[1]), bf),
            V((tok + 2 * WINDOW, k.shape[1]), bf), V((tok + 2 * WINDOW, k.shape[1]), bf),
            V((nb + 2, 8, WINDOW), jnp.int32),
            V((tok, q.shape[1]), bf), V((T, own, q.shape[1]), bf), V((T,) + w_out.shape, bf),
            V((own, d), f32), V((n_sp, tok, kb), bf), V((tok, ff), f32), V((tok, ff), f32), V((tok, ff), bf),
            V((n_sp, tok, kb), bf), V((T, n_sp, own, kb), bf),
            dma((4,)), dma((6,)), dma((6,)),
            dma((T,)), dma((T,)), dma((T,)), dma((T,)), dma((T,)), dma((T,)), dma((T,)), dma((T,)),
            dma((4, 1 + Y, Z)), dma((4, n_sp)), dma((2, n_sp)),
        ],
        compiler_params=params,
    )(*operands)


def solution(mesh):
    n_sp, T = mesh.shape["sp"], mesh.shape["tp"]
    Y = 2 if n_sp <= 8 else 4
    while n_sp % Y:
        Y //= 2
    placed = (
        P("sp", "tp"),
        P("sp", "tp"),
        P("sp", "tp"),
        P("sp"),
        P("tp"),
        P(("sp", "tp"), None),
        P("tp", None),
        P(),
        P("sp", "tp"),
        P("sp", "tp"),
        P("tp", "sp"),
    )
    return jax.shard_map(
        functools.partial(shards, n_sp // Y, Y, T), mesh=mesh, in_specs=placed,
        out_specs=P(("sp", "tp"), None), check_vma=False,
    )
```

```python
import functools

import jax
import jax.numpy as jnp
from jax import lax
from jax.experimental import pallas as pl
from jax.experimental.pallas import tpu as pltpu
from jax.sharding import PartitionSpec as P

HEAD = 64
WINDOW = 128
norm_eps = 1e-06
masked = -1e30
MESH = pl.DeviceIdType.MESH


def attend(n_sp, s, q_ref, k_ref, v_ref, drow_ref, dcol_ref, sink_ref, kext, vext, dext, att, wait_halo):
    tok = q_ref.shape[0]
    nb = tok // WINDOW
    heads = q_ref.shape[1] // HEAD
    groups = heads // (k_ref.shape[1] // HEAD)
    kext[pl.ds(WINDOW, tok)] = k_ref[...]
    vext[pl.ds(WINDOW, tok)] = v_ref[...]
    dext[pl.ds(1, nb)] = drow_ref[...]
    wait_halo()
    row_at = lax.broadcasted_iota(jnp.int32, (WINDOW, 3 * WINDOW), 0)
    col_at = lax.broadcasted_iota(jnp.int32, (WINDOW, 3 * WINDOW), 1) - WINDOW
    near = jnp.abs(row_at - col_at) <= WINDOW

    @pl.loop(0, nb)
    def _(blk):
        base = pl.multiple_of(blk * WINDOW, WINDOW)
        place = s * tok + base + col_at
        key_docs = jnp.concatenate([dext[blk + i][0:1] for i in range(3)], axis=1)
        query_docs = dcol_ref[pl.ds(base, WINDOW), 0:1]
        valid = near & (place >= 0) & (place < tok * n_sp) & (query_docs == key_docs)
        qs = q_ref[pl.ds(base, WINDOW)]
        ks = kext[pl.ds(base, 3 * WINDOW)]
        vs = vext[pl.ds(base, 3 * WINDOW)]
        outs = []
        for h in range(heads):
            g = h // groups
            scores = lax.dot_general(
                qs[:, h * HEAD:(h + 1) * HEAD], ks[:, g * HEAD:(g + 1) * HEAD],
                (((1,), (1,)), ((), ())), preferred_element_type=jnp.float32,
            ) * HEAD ** (-0.5)
            scores = jnp.where(valid, scores, masked)
            sink = sink_ref[h]
            top = jnp.maximum(jnp.max(scores, axis=-1, keepdims=True), sink)
            expd = jnp.exp(scores - top)
            total = jnp.sum(expd, axis=-1, keepdims=True) + jnp.exp(sink - top)
            probs = (expd / total).astype(jnp.bfloat16)
            outs.append(jnp.dot(probs, vs[:, g * HEAD:(g + 1) * HEAD], preferred_element_type=jnp.float32))
        att[pl.ds(base, WINDOW)] = jnp.concatenate(outs, axis=1).astype(jnp.bfloat16)


def kernel(
    Z, Y, T,
    q_ref, k_ref, v_ref, drow_ref, dcol_ref, sink_ref, resid_ref, gain_ref, wo_hbm, wg_hbm, wu_hbm, wd_hbm,
    out_ref,
    G, U, D, kext, vext, dext, att, rows, WO, mid, NB, gacc, uacc, hid, PT, RT,
    loc_sem, halo_s, halo_r, wo_s, wo_r, at_s, at_r, nb_s, nb_r, pt_s, pt_r, w_s, w_r, b_s,
):
    n_sp = Z * Y
    s, t = lax.axis_index("sp"), lax.axis_index("tp")
    z, y = s // Y, s % Y
    tok = q_ref.shape[0]
    nb = tok // WINDOW
    own = tok // T
    kb = G.shape[1]
    half = D.shape[1] // 2

    def rcopy(src, dst, ssem, rsem, sp_to, tp_to):
        return pltpu.make_async_remote_copy(
            src_ref=src, dst_ref=dst, send_sem=ssem, recv_sem=rsem,
            device_id={"sp": sp_to, "tp": tp_to}, device_id_type=MESH,
        )

    def arrived(ref, sem):
        pltpu.make_async_copy(ref, ref, sem).wait()

    def piece(m, slot):
        if m < 2:
            return (G, U)[m].at[slot]
        return D.at[slot, pl.ds(half if m == 2 else 0, half)]

    locals_ = [
        pltpu.make_async_copy(wd_hbm, D.at[s], loc_sem.at[2]),
        pltpu.make_async_copy(wg_hbm, G.at[s], loc_sem.at[0]),
        pltpu.make_async_copy(wu_hbm, U.at[s], loc_sem.at[1]),
        pltpu.make_async_copy(wo_hbm, WO.at[t], loc_sem.at[3]),
    ]
    for c in locals_:
        c.start()

    right, left = (s + 1) % n_sp, (s + n_sp - 1) % n_sp
    halos = []
    for i, (src, dst) in enumerate(((k_ref, kext), (v_ref, vext))):
        halos.append((src.at[pl.ds(tok - WINDOW, WINDOW)], dst.at[pl.ds(0, WINDOW)], 2 * i, right))
        halos.append((src.at[pl.ds(0, WINDOW)], dst.at[pl.ds(tok + WINDOW, WINDOW)], 2 * i + 1, left))
    halos.append((drow_ref.at[nb - 1], dext.at[0], 4, right))
    halos.append((drow_ref.at[0], dext.at[nb + 1], 5, left))
    halo_copies = [rcopy(a, b, halo_s.at[i], halo_r.at[i], to, t) for a, b, i, to in halos]
    for c in halo_copies:
        c.start()

    def up_copy(m, slot, sem):
        return rcopy(piece(m, slot), piece(m, slot), sem, w_r.at[m, slot], s + Y, t)

    def down_copy(m, slot, sem):
        return rcopy(piece(m, slot), piece(m, slot), sem, w_r.at[m, slot], s - Y, t)

    def z_sem(m, way, zz, yy):
        return b_s.at[way, zz * Y + yy] if m == 3 else w_s.at[m, way, zz]

    def send_up(m, zz, yy):
        @pl.when(z + 1 < Z)
        def _():
            up_copy(m, zz * Y + yy, z_sem(m, 0, zz, yy)).start()

    def send_down(m, zz, yy):
        @pl.when(z > 0)
        def _():
            down_copy(m, zz * Y + yy, z_sem(m, 1, zz, yy)).start()

    def y_copies(m, zz):
        slot = zz * Y + y
        return [
            rcopy(piece(m, slot), piece(m, slot), w_s.at[m, 1 + j, zz], w_r.at[m, slot], z * Y + (y + j) % Y, t)
            for j in range(1, Y)
        ]

    def send_y(m, zz):
        for c in y_copies(m, zz):
            c.start()

    def tp_peers():
        return [(t + j) % T for j in range(1, T)]

    for c in locals_[:1]:
        c.wait()
    send_y(3, z)
    for m in (0, 1):
        locals_[1 + m].wait()
        send_up(m, z, y)
        send_down(m, z, y)
        send_y(m, z)
    locals_[3].wait()
    wo_copies = [rcopy(WO.at[t], WO.at[t], wo_s.at[j], wo_r.at[t], s, p) for j, p in enumerate(tp_peers())]
    for c in wo_copies:
        c.start()

    attend(
        n_sp, s, q_ref, k_ref, v_ref, drow_ref, dcol_ref, sink_ref, kext, vext, dext, att,
        lambda: [arrived(b, halo_r.at[i]) for a, b, i, to in halos],
    )

    at_copies = [
        rcopy(att.at[pl.ds(pl.multiple_of(p * own, own), own)], rows.at[t], at_s.at[j], at_r.at[t], s, p)
        for j, p in enumerate(tp_peers())
    ]
    for c in at_copies:
        c.start()
    rows[t] = att[pl.ds(pl.multiple_of(t * own, own), own)]

    def handle(ms, r):
        for m in ms:
            for sign in (-1, 1):
                zz = z + sign * r

                @pl.when((zz >= 0) & (zz < Z))
                def _():
                    send = send_up if sign < 0 else send_down
                    columns = range(Y) if m == 3 else (0,)
                    for j in columns:
                        yy = (y + j) % Y
                        arrived(piece(m, zz * Y + yy), w_r.at[m, zz * Y + yy])
                        send(m, zz, yy)
                    if m != 3:
                        send_y(m, zz)

    def project():
        for p in tp_peers():
            arrived(WO.at[p], wo_r.at[p])
            arrived(rows.at[p], at_r.at[p])
        middle = resid_ref[...].astype(jnp.float32)
        for i in range(T):
            middle = middle + jnp.dot(rows[i], WO[i], preferred_element_type=jnp.float32)
        mid[...] = middle
        normed = (
            middle * lax.rsqrt(jnp.mean(middle * middle, axis=-1, keepdims=True) + norm_eps) * gain_ref[...]
        ).astype(jnp.bfloat16)
        mine = pl.ds(pl.multiple_of(t * own, own), own)
        for i in range(n_sp):
            NB[i, mine] = normed[:, i * kb:(i + 1) * kb]
        for c in nb_copies():
            c.start()

    def nb_rows(p):
        return NB.at[:, pl.ds(pl.multiple_of(p * own, own), own)]

    def nb_copies():
        return [rcopy(nb_rows(t), nb_rows(t), nb_s.at[j], nb_r.at[t], s, p) for j, p in enumerate(tp_peers())]

    step = min(tok, 256)

    def each(r, body):
        @pl.loop(0, (2 if r else 1) * Y)
        def _(i):
            joff = i % Y
            zz = z + (2 * (i // Y) - 1) * r
            slot = zz * Y + (y + joff) % Y

            @pl.when((zz >= 0) & (zz < Z))
            def _():
                body(slot, joff)

    def gate_up(r):
        def body(slot, joff):
            @pl.when(joff > 0)
            def _():
                for m in (0, 1):
                    arrived(piece(m, slot), w_r.at[m, slot])

            @pl.loop(0, tok // step)
            def _(i):
                at = pl.ds(pl.multiple_of(i * step, step), step)
                x = NB[slot, at]
                gacc[at] += jnp.dot(x, G[slot], preferred_element_type=jnp.float32)
                uacc[at] += jnp.dot(x, U[slot], preferred_element_type=jnp.float32)

        each(r, body)

    def pt_rows(slot, p):
        return PT.at[slot, pl.ds(pl.multiple_of(p * own, own), own)]

    def down(r):
        def body(slot, joff):
            @pl.when(joff > 0)
            def _():
                arrived(piece(2, slot), w_r.at[2, slot])

            @pl.loop(0, tok // step)
            def _(i):
                at = pl.ds(pl.multiple_of(i * step, step), step)
                PT[slot, at] = jnp.dot(hid[at], D[slot], preferred_element_type=jnp.float32).astype(jnp.bfloat16)

            for j, p in enumerate(tp_peers()):
                rcopy(pt_rows(slot, p), RT.at[t, slot], pt_s.at[j], pt_r.at[t], s, p).start()

        each(r, body)

    gacc[...] = jnp.zeros_like(gacc)
    uacc[...] = jnp.zeros_like(uacc)
    if Z > 1:
        handle((0, 1), 1)
    project()
    if Z > 2:
        handle((0, 1), 2)
    for p in tp_peers():
        arrived(nb_rows(p), nb_r.at[p])
    gate_up(0)
    for r in range(3, Z):
        handle((0, 1), r)
        gate_up(r - 2)

    for j in range(1, Y):
        slot = z * Y + (y + j) % Y
        arrived(piece(3, slot), w_r.at[3, slot])
    send_up(2, z, y)
    send_down(2, z, y)
    send_y(2, z)
    for j in range(Y):
        send_up(3, z, (y + j) % Y)
        send_down(3, z, (y + j) % Y)
    for r in range(max(1, Z - 2), Z - 1):
        gate_up(r)
    if Z > 1:
        handle((2, 3), 1)
        gate_up(Z - 1)

    @pl.loop(0, tok // WINDOW)
    def _(i):
        at = pl.ds(pl.multiple_of(i * WINDOW, WINDOW), WINDOW)
        gate = gacc[at]
        hid[at] = (gate / (1.0 + jnp.exp(-gate)) * uacc[at]).astype(jnp.bfloat16)

    down(0)
    for r in range(1, Z):
        if r + 1 < Z:
            handle((2, 3), r + 1)
        down(r)

    for p in tp_peers():
        arrived(RT.at[p], pt_r.at[p])
    for i in range(n_sp):
        cols = slice(i * kb, (i + 1) * kb)
        total = mid[:, cols] + PT[i, pl.ds(pl.multiple_of(t * own, own), own)].astype(jnp.float32)
        for p in tp_peers():
            total = total + RT[p, i].astype(jnp.float32)
        out_ref[:, cols] = total.astype(jnp.bfloat16)

    for c in halo_copies + wo_copies + at_copies + nb_copies():
        c.wait_send()
    for j, p in enumerate(tp_peers()):
        arrived(PT.at[:, pl.ds(pl.multiple_of(p * own, own), own)], pt_s.at[j])
    for c in y_copies(3, z):
        c.wait_send()
    for zz in range(Z):
        for m in range(3):
            for c in y_copies(m, zz):
                c.wait_send()
        for m in range(4):
            for j in range(Y if m == 3 else 1):
                yy = (y + j) % Y

                @pl.when((zz <= z) & (z + 1 < Z))
                def _():
                    up_copy(m, zz * Y + yy, z_sem(m, 0, zz, yy)).wait_send()

                @pl.when((zz >= z) & (z > 0))
                def _():
                    down_copy(m, zz * Y + yy, z_sem(m, 1, zz, yy)).wait_send()


def paired_kernel(
    Z, Y, T, W,
    q_ref, k_ref, v_ref, drow_ref, dcol_ref, sink_ref, resid_ref, gain_ref, wo_hbm, wg_hbm, wu_hbm, wd_hbm,
    out_ref,
    G, U, D, kext, vext, dext, att, rows, WO, mid, NB, gacc, uacc, hid, PT, RD, XS, RT, ZS, ZR,
    loc_sem, halo_s, halo_r, wo_s, wo_r, at_s, at_r, nb_s, nb_r, pt_s, pt_r, xs_s, xs_r, zs_s, zs_r, z_s, y_s, w_r,
):
    n_sp = Z * Y
    s, t = lax.axis_index("sp"), lax.axis_index("tp")
    z, y, x, core = s // Y, s % Y, t // 2, t % 2
    par = z % 2
    s_pair = (z + 1 - 2 * par) * Y + y
    t_pair = x * 2 + 1 - core
    tok = q_ref.shape[0]
    nb = tok // WINDOW
    own = tok // T
    all_tok = 2 * tok
    kb = G.shape[1]
    half = D.shape[1]
    offset = wg_hbm.shape[1] - W
    sent = []

    def rcopy(src, dst, ssem, rsem, sp_to, tp_to):
        return pltpu.make_async_remote_copy(
            src_ref=src, dst_ref=dst, send_sem=ssem, recv_sem=rsem,
            device_id={"sp": sp_to, "tp": tp_to}, device_id_type=MESH,
        )

    def push(*parts):
        c = rcopy(*parts)
        c.start()
        sent.append(c)

    def arrived(ref, sem):
        pltpu.make_async_copy(ref, ref, sem).wait()

    def source(m, which):
        if m < 2:
            return (wg_hbm, wu_hbm)[m].at[:, pl.ds(pl.multiple_of(which * offset, 128), W)]
        return wd_hbm.at[pl.ds(pl.multiple_of(which * half, 16), half)]

    def piece(m, slot):
        return (G, U, D)[m].at[slot]

    def tp_peers():
        return [(t + j) % T for j in range(1, T)]

    def x_peers():
        return [((x + j) % (T // 2)) * 2 + core for j in range(1, T // 2)]

    right, left = (s + 1) % n_sp, (s + n_sp - 1) % n_sp
    halos = []
    for i, (src, dst) in enumerate(((k_ref, kext), (v_ref, vext))):
        halos.append((src.at[pl.ds(tok - WINDOW, WINDOW)], dst.at[pl.ds(0, WINDOW)], 2 * i, right))
        halos.append((src.at[pl.ds(0, WINDOW)], dst.at[pl.ds(tok + WINDOW, WINDOW)], 2 * i + 1, left))
    halos.append((drow_ref.at[nb - 1], dext.at[0], 4, right))
    halos.append((drow_ref.at[0], dext.at[nb + 1], 5, left))
    for a, b, i, to in halos:
        push(a, b, halo_s.at[i], halo_r.at[i], to, t)

    locals_ = [pltpu.make_async_copy(source(m, par), piece(m, s), loc_sem.at[m]) for m in range(3)]
    locals_.append(pltpu.make_async_copy(wo_hbm, WO.at[t], loc_sem.at[3]))
    for c in locals_:
        c.start()

    def z_copy(m, zz):
        return rcopy(source(m, zz % 2), piece(m, s), z_s.at[m, zz], w_r.at[m, s], zz * Y + y, t)

    def send_z(m, r):
        for sign in (-1, 1):
            zz = z + sign * r

            @pl.when((zz >= 0) & (zz < Z))
            def _():
                z_copy(m, zz).start()

    def y_copies(m, zz):
        slot = zz * Y + y
        return [
            rcopy(piece(m, slot), piece(m, slot), y_s.at[m, j, zz], w_r.at[m, slot], z * Y + (y + j) % Y, t)
            for j in range(1, Y)
        ]

    def send_y(m, zz):
        for c in y_copies(m, zz):
            c.start()

    def handle(ms, r):
        for m in ms:
            for sign in (-1, 1):
                zz = z + sign * r

                @pl.when((zz >= 0) & (zz < Z))
                def _():
                    arrived(piece(m, zz * Y + y), w_r.at[m, zz * Y + y])
                    send_y(m, zz)

    for r in range(1, max(2, Z - 1)):
        for m in (0, 1):
            send_z(m, r)
    for m in (0, 1):
        locals_[m].wait()
        send_y(m, z)
    locals_[2].wait()
    locals_[3].wait()
    for j, p in enumerate(x_peers() + [t_pair]):
        push(WO.at[t], WO.at[t], wo_s.at[j], wo_r.at[t], s, p)

    attend(
        Z * Y, s, q_ref, k_ref, v_ref, drow_ref, dcol_ref, sink_ref, kext, vext, dext, att,
        lambda: [arrived(b, halo_r.at[i]) for a, b, i, to in halos],
    )
    for j, p in enumerate(tp_peers()):
        push(att.at[pl.ds(pl.multiple_of(p * own, own), own)], rows.at[t], at_s.at[j], at_r.at[t], s, p)
    rows[t] = att[pl.ds(pl.multiple_of(t * own, own), own)]

    handle((0, 1), 1)

    for j, p in enumerate(x_peers()):
        arrived(WO.at[p], wo_r.at[p])
        push(WO.at[p], WO.at[p], wo_s.at[T // 2 + j], wo_r.at[p], s, t_pair)
    for p in [t_pair] + [(p // 2) * 2 + 1 - core for p in x_peers()]:
        arrived(WO.at[p], wo_r.at[p])
    for p in tp_peers():
        arrived(rows.at[p], at_r.at[p])
    middle = resid_ref[...].astype(jnp.float32)
    for i in range(T):
        middle = middle + jnp.dot(rows[i], WO[i], preferred_element_type=jnp.float32)
    mid[...] = middle
    normed = (
        middle * lax.rsqrt(jnp.mean(middle * middle, axis=-1, keepdims=True) + norm_eps) * gain_ref[...]
    ).astype(jnp.bfloat16)

    def at_rows(p, which):
        return pl.ds(pl.multiple_of((p * 2 + which) * own, own), own)

    for i in range(n_sp):
        NB[i, at_rows(t, par)] = normed[:, i * kb:(i + 1) * kb]

    def push_rows(p, which, k, sp_to, tp_to):
        part = NB.at[:, at_rows(p, which)]
        push(part, part, nb_s.at[k], nb_r.at[p, which], sp_to, tp_to)

    def wait_rows(p, which):
        arrived(NB.at[:, at_rows(p, which)], nb_r.at[p, which])

    n_x = T // 2
    push_rows(t, par, 0, s_pair, t)
    for j, p in enumerate(x_peers() + [t_pair]):
        push_rows(t, par, 1 + j, s, p)
    for r in range(max(2, Z - 1), Z):
        for m in (0, 1):
            send_z(m, r)
    for r in range(1, Z):
        send_z(2, r)
    for r in range(2, max(3, Z - 1)):
        if r < Z:
            handle((0, 1), r)
    wait_rows(t, 1 - par)
    for j, p in enumerate(x_peers() + [t_pair]):
        push_rows(t, 1 - par, 1 + n_x + j, s, p)
    for r in range(max(3, Z - 1), Z):
        handle((0, 1), r)
    send_y(2, z)
    for j, p in enumerate(x_peers()):
        for i, which in enumerate((par, 1 - par)):
            wait_rows(p, which)
            push_rows(p, which, 1 + 2 * n_x + 2 * j + i, s, t_pair)
    for p in [t_pair] + [(p // 2) * 2 + 1 - core for p in x_peers()]:
        for which in (par, 1 - par):
            wait_rows(p, which)

    step = min(all_tok, 256)

    def each(r, body):
        @pl.loop(0, (2 if r else 1) * Y)
        def _(i):
            joff = i % Y
            zz = z + (2 * (i // Y) - 1) * r
            slot = zz * Y + (y + joff) % Y

            @pl.when((zz >= 0) & (zz < Z))
            def _():
                body(slot, joff)

    def gate_up(r):
        def body(slot, joff):
            @pl.when(joff > 0)
            def _():
                for m in (0, 1):
                    arrived(piece(m, slot), w_r.at[m, slot])

            @pl.loop(0, all_tok // step)
            def _(i):
                at = pl.ds(pl.multiple_of(i * step, step), step)
                rows_in = NB[slot, at]
                gacc[at] += jnp.dot(rows_in, G[slot], preferred_element_type=jnp.float32)
                uacc[at] += jnp.dot(rows_in, U[slot], preferred_element_type=jnp.float32)

        each(r, body)

    def peer_rows(p):
        return pl.ds(pl.multiple_of(p * 2 * own, 2 * own), 2 * own)

    def down(r):
        def body(slot, joff):
            @pl.when(joff > 0)
            def _():
                arrived(piece(2, slot), w_r.at[2, slot])

            @pl.loop(0, all_tok // step)
            def _(i):
                at = pl.ds(pl.multiple_of(i * step, step), step)
                PT[slot, at] = jnp.dot(hid[at], D[slot], preferred_element_type=jnp.float32).astype(jnp.bfloat16)

            for i in range(n_x):
                rows_out = PT.at[slot, peer_rows(i * 2 + 1 - core)]
                rcopy(rows_out, RD.at[slot, i], pt_s.at[i], pt_r.at[slot], s, t_pair).start()

        each(r, body)

    def mix(r):
        def body(slot, joff):
            arrived(RD.at[slot], pt_r.at[slot])
            for j, p in enumerate(x_peers()):
                both = PT[slot, peer_rows(p)].astype(jnp.float32) + RD[slot, p // 2].astype(jnp.float32)
                XS[slot, j] = both.astype(jnp.bfloat16)
                rcopy(XS.at[slot, j], RT.at[x, slot], xs_s.at[j], xs_r.at[x, slot], s, p).start()

        each(r, body)

    def reduce(r):
        def body(slot, joff):
            for p in x_peers():
                arrived(RT.at[p // 2, slot], xs_r.at[p // 2, slot])
            there = pl.ds(pl.multiple_of((1 - par) * own, own), own)
            away = PT[slot, at_rows(t, 1 - par)].astype(jnp.float32) + RD[slot, x, there].astype(jnp.float32)
            for p in x_peers():
                away = away + RT[p // 2, slot, there].astype(jnp.float32)
            ZS[slot] = away.astype(jnp.bfloat16)
            rcopy(ZS.at[slot], ZR.at[slot], zs_s, zs_r, s_pair, t).start()

        each(r, body)

    gacc[...] = jnp.zeros_like(gacc)
    uacc[...] = jnp.zeros_like(uacc)
    gate_up(0)
    gate_up(1)
    handle((2,), 1)
    for r in range(2, Z):
        gate_up(r)

    @pl.loop(0, all_tok // WINDOW)
    def _(i):
        at = pl.ds(pl.multiple_of(i * WINDOW, WINDOW), WINDOW)
        gate = gacc[at]
        act = (gate / (1.0 + jnp.exp(-gate)) * uacc[at]).astype(jnp.bfloat16)

        @pl.when(par == 0)
        def _():
            hid[at] = act[:, :half]

        @pl.when(par == 1)
        def _():
            hid[at] = act[:, W - half:]

    down(0)
    for r in range(1, Z):
        if r + 1 < Z:
            handle((2,), r + 1)
        down(r)
        mix(r - 1)
        if r > 1:
            reduce(r - 2)
    mix(Z - 1)
    for r in range(max(0, Z - 2), Z):
        reduce(r)

    arrived(ZR, zs_r)
    here = pl.ds(pl.multiple_of(par * own, own), own)
    for i in range(n_sp):
        cols = slice(i * kb, (i + 1) * kb)
        total = mid[:, cols] + PT[i, at_rows(t, par)].astype(jnp.float32) + ZR[i].astype(jnp.float32)
        total = total + RD[i, x, here].astype(jnp.float32)
        for p in x_peers():
            total = total + RT[p // 2, i, here].astype(jnp.float32)
        out_ref[:, cols] = total.astype(jnp.bfloat16)

    for c in sent:
        c.wait_send()
    for i in range(n_x):
        arrived(PT.at[:, peer_rows(i * 2 + 1 - core)], pt_s.at[i])
    for j in range(n_x - 1):
        arrived(XS.at[:, j], xs_s.at[j])
    arrived(ZS, zs_s)
    for m in range(3):
        for zz in range(Z):
            for c in y_copies(m, zz):
                c.wait_send()

            @pl.when(z != zz)
            def _():
                z_copy(m, zz).wait_send()


def shards(Z, Y, T, q, k, v, doc_ids, sinks, resid, w_out, gain, wg, wu, wd):
    n_sp = Z * Y
    tok, (kb, ff), d = q.shape[0], wg.shape, resid.shape[1]
    nb, own = tok // WINDOW, tok // T
    bf, f32 = jnp.bfloat16, jnp.float32
    drow = jnp.broadcast_to(doc_ids.reshape(nb, 1, WINDOW), (nb, 8, WINDOW))
    dcol = jnp.broadcast_to(doc_ids[:, None], (tok, 128))
    vmem, hbm = pl.BlockSpec(memory_space=pltpu.VMEM), pl.BlockSpec(memory_space=pl.ANY)
    dma = pltpu.SemaphoreType.DMA
    V = pltpu.VMEM
    specs = [vmem] * 5 + [pl.BlockSpec(memory_space=pltpu.SMEM)] + [vmem] * 2 + [hbm] * 4
    params = pltpu.CompilerParams(has_side_effects=True, vmem_limit_bytes=60 * 1024 * 1024)
    operands = (q, k, v, drow, dcol, sinks, resid, gain.reshape(1, d), w_out, wg, wu, wd)
    half = ff // 2
    W = -(-half // 128) * 128
    if Z % 2 == 0 and T % 2 == 0 and (ff - W) % 128 == 0 and half % 16 == 0 and kb % 128 == 0:
        return pl.pallas_call(
            functools.partial(paired_kernel, Z, Y, T, W),
            out_shape=jax.ShapeDtypeStruct((own, d), bf),
            in_specs=specs,
            out_specs=vmem,
            scratch_shapes=[
                V((n_sp, kb, W), bf), V((n_sp, kb, W), bf), V((n_sp, half, wd.shape[1]), bf),
                V((tok + 2 * WINDOW, k.shape[1]), bf), V((tok + 2 * WINDOW, k.shape[1]), bf),
                V((nb + 2, 8, WINDOW), jnp.int32),
                V((tok, q.shape[1]), bf), V((T, own, q.shape[1]), bf), V((T,) + w_out.shape, bf),
                V((own, d), f32), V((n_sp, 2 * tok, kb), bf),
                V((2 * tok, W), f32), V((2 * tok, W), f32), V((2 * tok, half), bf),
                V((n_sp, 2 * tok, kb), bf), V((n_sp, T // 2, 2 * own, kb), bf),
                V((n_sp, max(1, T // 2 - 1), 2 * own, kb), bf), V((T // 2, n_sp, 2 * own, kb), bf),
                V((n_sp, own, kb), bf), V((n_sp, own, kb), bf),
                dma((4,)), dma((6,)), dma((6,)),
                dma((T,)), dma((T,)), dma((T,)), dma((T,)), dma((2 * T + 1,)), dma((T, 2)),
                dma((T,)), dma((n_sp,)), dma((T,)), dma((T, n_sp)), dma(()), dma(()),
                dma((3, Z)), dma((3, Y, Z)), dma((3, n_sp)),
            ],
            compiler_params=params,
        )(*operands)
    return pl.pallas_call(
        functools.partial(kernel, Z, Y, T),
        out_shape=jax.ShapeDtypeStruct((own, d), bf),
        in_specs=specs,
        out_specs=vmem,
        scratch_shapes=[
            V((n_sp, kb, ff), bf), V((n_sp, kb, ff), bf), V((n_sp, ff, wd.shape[1]), bf),
            V((tok + 2 * WINDOW, k.shape[1]), bf), V((tok + 2 * WINDOW, k.shape[1]), bf),
            V((nb + 2, 8, WINDOW), jnp.int32),
            V((tok, q.shape[1]), bf), V((T, own, q.shape[1]), bf), V((T,) + w_out.shape, bf),
            V((own, d), f32), V((n_sp, tok, kb), bf), V((tok, ff), f32), V((tok, ff), f32), V((tok, ff), bf),
            V((n_sp, tok, kb), bf), V((T, n_sp, own, kb), bf),
            dma((4,)), dma((6,)), dma((6,)),
            dma((T,)), dma((T,)), dma((T,)), dma((T,)), dma((T,)), dma((T,)), dma((T,)), dma((T,)),
            dma((4, 1 + Y, Z)), dma((4, n_sp)), dma((2, n_sp)),
        ],
        compiler_params=params,
    )(*operands)


def solution(mesh):
    n_sp, T = mesh.shape["sp"], mesh.shape["tp"]
    Y = 2 if n_sp <= 8 else 4
    while n_sp % Y:
        Y //= 2
    placed = (
        P("sp", "tp"),
        P("sp", "tp"),
        P("sp", "tp"),
        P("sp"),
        P("tp"),
        P(("sp", "tp"), None),
        P("tp", None),
        P(),
        P("sp", "tp"),
        P("sp", "tp"),
        P("tp", "sp"),
    )
    return jax.shard_map(
        functools.partial(shards, n_sp // Y, Y, T), mesh=mesh, in_specs=placed,
        out_specs=P(("sp", "tp"), None), check_vma=False,
    )
```
